32 devices in a mesh: fs: 8 (over z, x), tp: 4 (over y, core).
Axes of the slice: x: 2, y: 2, z: 4, core: 2. Of those that a mesh axis runs over, the one named last changes fastest.
Arguments:
- tokens: bfloat16 [2048, 3072], P('tp', 'fs'), may hold values from -6 to 6
- mix_gain: float32 [2048], replicated, may hold values from 0.1 to 1.9
- mlp_gain: float32 [2048], replicated, may hold values from 0.1 to 1.9
- query_weight: float32 [2048, 1024], P('fs', 'tp'), may hold values from -0.125 to 0.125
- key_weight: float32 [2048, 1024], P('fs', 'tp'), may hold values from -0.125 to 0.125
- value_weight: float32 [2048, 1024], P('fs', 'tp'), may hold values from -0.125 to 0.125
- gate_weight: float32 [2048, 1024], P('fs', 'tp'), may hold values from -0.125 to 0.125
- out_weight: float32 [1024, 2048], P('tp', 'fs'), may hold values from -0.1875 to 0.1875
- up_weight: float32 [2048, 8192], P('fs', 'tp'), may hold values from -0.125 to 0.125
- down_weight: float32 [8192, 2048], P('tp', 'fs'), may hold values from -0.0625 to 0.0625
- query_scale: float32 [1024], P(('tp', 'fs')), may hold values from 0.1 to 1.9
- key_scale: float32 [1024], P(('tp', 'fs')), may hold values from 0.1 to 1.9
- value_scale: float32 [1024], P(('tp', 'fs')), may hold values from 0.1 to 1.9
- gate_scale: float32 [1024], P(('tp', 'fs')), may hold values from 0.1 to 1.9
- out_scale: float32 [2048], P(('tp', 'fs')), may hold values from 0.1 to 1.9
- up_scale: float32 [8192], P(('tp', 'fs')), may hold values from 0.1 to 1.9
- down_scale: float32 [2048], P(('tp', 'fs')), may hold values from 0.1 to 1.9
- forget: float32 [16], P('tp'), as said below
Outputs:
- layer_out: bfloat16 [2048, 3072], P('tp', 'fs')
The draws below stay inside these ranges and needn't reach their ends.
Inputs may be any that keep to these rules, and one draw needn't show every extreme that they name: `forget`: positive rates; each head either forgets within a few tens of positions or keeps a tenth or more over a whole sequence of 384.
All inputs are finite; a program needn't handle non-finite values.
Results may differ from the reference program's by a relative error of at most 0.02.
Values may be sent and summed in bfloat16 or wider, within the bound.
A program may use at most 64 MiB of HBM per device.

```python
import math
import jax
import jax.numpy as jnp
from jax import lax

D = 2048
HEADS = 16
HEAD_DIM = 64
FF = 8192
LEN = 384
RET_W = 1024
TOKENS = 3072
N_FS = 8
N_TP = 4


def draw_forget(key, part):
    first, second, third = jax.random.split(key, 3)
    fast = jax.random.randint(first, (HEADS,), 0, 16) < 8
    quick = jax.random.uniform(second, (HEADS,), jnp.float32, 1.0 / 50.0, 1.0 / 25.0)
    slow = jnp.exp(jax.random.uniform(third, (HEADS,), jnp.float32, math.log(0.1 / LEN), math.log(2.0 / LEN)))
    return jnp.where(fast, quick, slow).astype(jnp.float32)


def shard_levels(key, dims, cuts, smallest, largest):
    factor_of, own = 1.0, jax.random.fold_in(key, 6)
    for dim, shards_of in cuts:
        draws = jnp.exp(jax.random.uniform(jax.random.fold_in(own, dim), (shards_of,), jnp.float32, smallest / len(cuts), largest / len(cuts)))
        factor_of = factor_of * jnp.repeat(draws, dims[dim] // shards_of).reshape([-1 if axis == dim else 1 for axis in range(len(dims))])
    return factor_of


def centred(rng, extent, deviation, limit, cuts=(), held_as=jnp.bfloat16):
    array = deviation * jax.random.normal(rng, extent, jnp.float32)
    if cuts:
        array = array * shard_levels(rng, extent, cuts, -0.22, 0.18)
    return jnp.clip(array, -limit, limit).astype(held_as)


def setup_inputs(seed: int = 0) -> dict:
    key_list = jax.random.split(jax.random.key(seed), 19)
    tokens = centred(key_list[0], (D, TOKENS), 1.0, 6.0, ((0, 4), (1, 8)))
    mix_gain = jnp.clip(1.0 + 0.18 * jax.random.normal(key_list[1], (D,), jnp.float32), 0.1, 1.9)
    mlp_gain = jnp.clip(1.0 + 0.18 * jax.random.normal(key_list[2], (D,), jnp.float32), 0.1, 1.9)
    query_weight = centred(key_list[3], (D, RET_W), D ** -0.5, 0.125, ((0, 8), (1, 4)), jnp.float32)
    key_weight = centred(key_list[4], (D, RET_W), D ** -0.5, 0.125, ((0, 8), (1, 4)), jnp.float32)
    value_weight = centred(key_list[5], (D, RET_W), D ** -0.5, 0.125, ((0, 8), (1, 4)), jnp.float32)
    gate_weight = centred(key_list[6], (D, RET_W), D ** -0.5, 0.125, ((0, 8), (1, 4)), jnp.float32)
    out_weight = centred(key_list[7], (RET_W, D), RET_W ** -0.5, 0.1875, ((0, 4), (1, 8)), jnp.float32)
    up_weight = centred(key_list[8], (D, FF), D ** -0.5, 0.125, ((0, 8), (1, 4)), jnp.float32)
    down_weight = centred(key_list[9], (FF, D), FF ** -0.5, 0.0625, ((0, 4), (1, 8)), jnp.float32)
    query_scale = jnp.clip(1.0 + 0.18 * jax.random.normal(key_list[10], (RET_W,), jnp.float32), 0.1, 1.9)
    key_scale = jnp.clip(1.0 + 0.18 * jax.random.normal(key_list[11], (RET_W,), jnp.float32), 0.1, 1.9)
    value_scale = jnp.clip(1.0 + 0.18 * jax.random.normal(key_list[12], (RET_W,), jnp.float32), 0.1, 1.9)
    gate_scale = jnp.clip(1.0 + 0.18 * jax.random.normal(key_list[13], (RET_W,), jnp.float32), 0.1, 1.9)
    out_scale = jnp.clip(1.0 + 0.18 * jax.random.normal(key_list[14], (D,), jnp.float32), 0.1, 1.9)
    up_scale = jnp.clip(1.0 + 0.18 * jax.random.normal(key_list[15], (FF,), jnp.float32), 0.1, 1.9)
    down_scale = jnp.clip(1.0 + 0.18 * jax.random.normal(key_list[16], (D,), jnp.float32), 0.1, 1.9)
    forget = draw_forget(jax.random.fold_in(key_list[18], 71), 0)
    return dict(tokens=tokens, mix_gain=mix_gain, mlp_gain=mlp_gain, query_weight=query_weight, key_weight=key_weight, value_weight=value_weight, gate_weight=gate_weight, out_weight=out_weight, up_weight=up_weight, down_weight=down_weight, query_scale=query_scale, key_scale=key_scale, value_scale=value_scale, gate_scale=gate_scale, out_scale=out_scale, up_scale=up_scale, down_scale=down_scale, forget=forget)


def rotary(field, pos):
    half = field.shape[-1] // 2
    inverse = 1.0 / 10000.0 ** jnp.linspace(0.0, 1.0, half, dtype=jnp.float32)
    angle = pos[:, None] * inverse[None, :]
    cosine = jnp.cos(angle)[None, :, None, :]
    sine = jnp.sin(angle)[None, :, None, :]
    paired = field.astype(jnp.float32).reshape(field.shape[:-1] + (half, 2))
    first, second = (paired[..., 0], paired[..., 1])
    turned = jnp.stack([first * cosine - second * sine, first * sine + second * cosine], axis=-1)
    return turned.reshape(field.shape)

def retain(query, key, value, gate, forget):
    batch, length, heads, width = query.shape
    block = 128
    count = length // block
    top = lax.Precision.HIGHEST
    pos = jnp.arange(length, dtype=jnp.float32)
    rot_q = rotary(query, pos)
    rot_k = rotary(key, pos) * width ** (-0.5)
    vals = value.astype(jnp.float32)
    log_decay = -forget.astype(jnp.float32)
    steps = jnp.arange(block, dtype=jnp.float32)
    offset = steps[:, None] - steps[None, :]
    decay_mask = jnp.where(offset >= 0, jnp.exp(log_decay[:, None, None] * jnp.maximum(offset, 0.0)), 0.0)
    q_blocks = rot_q.reshape(batch, count, block, heads, width)
    k_blocks = rot_k.reshape(batch, count, block, heads, width)
    v_blocks = vals.reshape(batch, count, block, heads, width)
    inner = jnp.einsum('bnihd,bnjhd->bnhij', q_blocks, k_blocks, precision=top) * decay_mask
    inner = jnp.einsum('bnhij,bnjhe->bnihe', inner, v_blocks, precision=top)
    tail = jnp.exp(log_decay[:, None] * (block - 1.0 - steps)[None, :])
    update = jnp.einsum('bnjhd,bnjhe,hj->nbhde', k_blocks, v_blocks, tail, precision=top)
    block_decay = jnp.exp(log_decay * block)[None, :, None, None]

    def advance(state, piece):
        return (state * block_decay + piece, state)
    start_state = jnp.zeros((batch, heads, width, width), jnp.float32)
    _, before = lax.scan(advance, start_state, update)
    lead = jnp.exp(log_decay[None, :] * (steps[:, None] + 1.0))
    cross = jnp.einsum('bnihd,nbhde->bnihe', q_blocks, before, precision=top) * lead[None, None, :, :, None]
    total = inner + cross
    total = total * lax.rsqrt(lax.optimization_barrier(jnp.mean(total * total, axis=-1, keepdims=True)) + 0.01)
    total = total.reshape(batch, length, heads, width)
    return jax.nn.silu(gate.astype(jnp.float32)) * total

def norm_rows(rows, gain):
    scale = lax.rsqrt(lax.optimization_barrier(jnp.mean(rows * rows, axis=-1, keepdims=True)) + 1e-06)
    return (rows * scale * gain[None, :]).astype(jnp.bfloat16)

def reference(tokens, mix_gain, mlp_gain, query_weight, key_weight, value_weight, gate_weight, out_weight, up_weight, down_weight, query_scale, key_scale, value_scale, gate_scale, out_scale, up_scale, down_scale, forget):
    stream = tokens.astype(jnp.float32).T
    normed = norm_rows(stream, mix_gain)

    def project(weight, scale):
        product = jnp.dot(normed, weight.astype(jnp.bfloat16), preferred_element_type=jnp.float32)
        return (product * scale[None, :]).astype(jnp.bfloat16)
    shape = (N_FS, LEN, HEADS, HEAD_DIM)
    query = project(query_weight, query_scale).reshape(shape)
    key = project(key_weight, key_scale).reshape(shape)
    value = project(value_weight, value_scale).reshape(shape)
    gate = project(gate_weight, gate_scale).reshape(shape)
    mixed_heads = retain(query, key, value, gate, forget).reshape(TOKENS, RET_W).astype(jnp.bfloat16)
    out_b = out_weight.astype(jnp.bfloat16)
    group = RET_W // N_TP

    def mix_group(carry, index):
        rows = lax.dynamic_slice_in_dim(mixed_heads, index * group, group, 1)
        weight = lax.dynamic_slice_in_dim(out_b, index * group, group, 0)
        part = jnp.dot(rows, weight, preferred_element_type=jnp.float32).astype(jnp.bfloat16)
        part = lax.optimization_barrier(part)
        return (carry + part.astype(jnp.float32), None)
    groups = jnp.arange(N_TP, dtype=jnp.int32)
    mix_total, _ = lax.scan(mix_group, jnp.zeros((TOKENS, D), jnp.float32), groups)
    after_mix = (stream + mix_total * out_scale[None, :]).astype(jnp.bfloat16)
    normed_mlp = norm_rows(after_mix.astype(jnp.float32), mlp_gain)
    units = FF // N_TP

    def mlp_group(carry, index):
        w_up = lax.dynamic_slice_in_dim(up_weight, index * units, units, 1).astype(jnp.bfloat16)
        s_up = lax.dynamic_slice_in_dim(up_scale, index * units, units, 0)
        hidden = jnp.dot(normed_mlp, w_up, preferred_element_type=jnp.float32) * s_up[None, :]
        hidden = jnp.square(jax.nn.relu(hidden)).astype(jnp.bfloat16)
        w_down = lax.dynamic_slice_in_dim(down_weight, index * units, units, 0).astype(jnp.bfloat16)
        part = jnp.dot(hidden, w_down, preferred_element_type=jnp.float32).astype(jnp.bfloat16)
        part = lax.optimization_barrier(part)
        return (carry + part.astype(jnp.float32), None)
    mlp_total, _ = lax.scan(mlp_group, jnp.zeros((TOKENS, D), jnp.float32), groups)
    layer_out = (after_mix.astype(jnp.float32) + mlp_total * down_scale[None, :]).astype(jnp.bfloat16)
    return layer_out.T
```

```python
import functools

import jax
import jax.numpy as jnp
import numpy as np
from jax import lax
from jax.experimental import pallas as pl
from jax.experimental.pallas import tpu as pltpu
from jax.sharding import PartitionSpec as P

MESH = pl.DeviceIdType.MESH
BF = jnp.bfloat16
F32 = jnp.float32


def nn(a, b):
    return lax.dot_general(a, b, (((1,), (0,)), ((), ())), preferred_element_type=F32)


def nt(a, b):
    return lax.dot_general(a, b, (((1,), (1,)), ((), ())), preferred_element_type=F32)


def kernel(cfg, *refs):
    Z, X, n_tp, n_ch, heads = cfg
    n_fs = Z * X
    n_w = 2 + 2 * n_ch
    tok, gains, scales, cos_t, sin_t, forget = refs[:6]
    own = refs[6 : 6 + n_w]
    out_ref = refs[6 + n_w]
    rest = refs[7 + n_w :]
    full = rest[:n_w]
    (scale_g, tok_g, mix_p, mix_r, am_g, mlp_p, mlp_r, normed, proj, mixed, hidden, acc, scale_row,
     local_sem, zs, zr, xs, xr, ts, tr) = rest[n_w:]
    me = lax.axis_index("fs")
    tp = lax.axis_index("tp")
    z = me // X
    x = lax.rem(me, X)
    length, width = tok.shape
    ret = mixed.shape[1]
    head = ret // heads

    def at_z(o):
        return lax.rem(z + o, Z) * X + x

    def at_x(o):
        return z * X + lax.rem(x + o, X)

    def at_tp(o):
        return lax.rem(tp + o, n_tp)

    barrier = pltpu.get_barrier_semaphore()
    for o in range(1, Z):
        pl.semaphore_signal(barrier, inc=1, device_id={"fs": at_z(o)}, device_id_type=MESH)
    for o in range(1, X):
        pl.semaphore_signal(barrier, inc=1, device_id={"fs": at_x(o)}, device_id_type=MESH)
    for o in range(1, n_tp):
        pl.semaphore_signal(barrier, inc=1, device_id={"tp": at_tp(o)}, device_id_type=MESH)
    pl.semaphore_wait(barrier, Z - 1 + X - 1 + n_tp - 1)

    def place(w, owner):
        if w == n_w:
            return scale_g.at[owner]
        rows = own[w].shape[0]
        return full[w].at[pl.ds(pl.multiple_of(owner * rows, rows), rows)]

    def mine(w):
        return scales if w == n_w else own[w]

    pending = []

    def remote(src, dst, ss, rs, where):
        return pltpu.make_async_remote_copy(
            src_ref=src, dst_ref=dst, send_sem=ss, recv_sem=rs, device_id=where, device_id_type=MESH
        )

    def z_copy(w, o):
        return remote(mine(w), place(w, me), zs.at[w, o - 1], zr.at[w, o - 1], {"fs": at_z(o)})

    def z_send(w):
        for o in range(1, Z):
            copy = z_copy(w, o)
            copy.start()
            pending.append(copy)

    def x_own(w):
        for o in range(1, X):
            copy = remote(mine(w), place(w, me), xs.at[w, 0, o - 1], xr.at[w, 0, o - 1], {"fs": at_x(o)})
            copy.start()
            pending.append(copy)

    def relay(w):
        for k in range(1, Z):
            piece = place(w, at_z(Z - k))
            remote(mine(w), piece, zs.at[w, k - 1], zr.at[w, k - 1], {"fs": at_z(k)}).wait_recv()
            for o in range(1, X):
                copy = remote(piece, piece, xs.at[w, k, o - 1], xr.at[w, k, o - 1], {"fs": at_x(o)})
                copy.start()
                pending.append(copy)

    def finish(w):
        for k in range(Z):
            for o in range(1, X):
                owner = lax.rem(z + Z - k, Z) * X + lax.rem(x + X - o, X)
                piece = place(w, owner)
                remote(piece, piece, xs.at[w, k, o - 1], xr.at[w, k, o - 1], {"fs": at_x(o)}).wait_recv()

    def tp_copy(stage, src, dst, o):
        return remote(src, dst, ts.at[stage, o - 1], tr.at[stage, o - 1], {"tp": at_tp(o)})

    def tp_gather(stage, src, buffer):
        for o in range(1, n_tp):
            copy = tp_copy(stage, src, buffer.at[tp], o)
            copy.start()
            pending.append(copy)

    def tp_wait(stage, buffer):
        for o in range(1, n_tp):
            slot = buffer.at[at_tp(n_tp - o)]
            tp_copy(stage, slot, slot, o).wait_recv()

    def tp_scatter(stage, parts, buffer):
        for o in range(1, n_tp):
            copy = tp_copy(stage, parts.at[at_tp(o)], buffer.at[o - 1], o)
            copy.start()
            pending.append(copy)

    def tp_sum(stage, parts, buffer):
        total = parts[tp].astype(F32)
        for o in range(1, n_tp):
            tp_copy(stage, buffer.at[o - 1], buffer.at[o - 1], o).wait_recv()
            total += buffer[o - 1].astype(F32)
        return total

    def norm(buffer, row):
        square = jnp.zeros((length, 1), F32)
        for t in range(n_tp):
            v = buffer[t].astype(F32)
            square += jnp.sum(v * v, axis=-1, keepdims=True)
        factor = lax.rsqrt(square / (width * n_tp) + 1e-6)
        for t in range(n_tp):
            cols = slice(t * width, (t + 1) * width)
            normed[:, cols] = (buffer[t].astype(F32) * factor * gains[row : row + 1, cols]).astype(BF)

    ups = list(range(2, 2 + n_ch))
    downs = list(range(2 + n_ch, n_w))

    tp_gather(0, tok, tok_g)
    for w in [n_w, 0, 1]:
        z_send(w)
        x_own(w)
    for w in ups + downs:
        z_send(w)
    locals_ = [pltpu.make_async_copy(mine(w), place(w, me), local_sem.at[w]) for w in range(n_w + 1)]
    locals_.append(pltpu.make_async_copy(tok, tok_g.at[tp], local_sem.at[n_w + 1]))
    for copy in locals_:
        copy.start()
    for copy in locals_:
        copy.wait()
    tp_wait(0, tok_g)
    norm(tok_g, 0)

    relay(n_w)
    relay(0)
    x_own(ups[0])
    relay(1)
    for w in ups[1:]:
        x_own(w)
    finish(n_w)
    finish(0)
    scale = jnp.sum(scale_g[...], axis=0)
    scale_row[...] = scale
    at = 4 * ret
    out_scale = scale[:, at : at + width]
    down_scale = scale[:, at + width : at + 2 * width]
    up_at = at + 2 * width

    for i in range(4):
        piece = nn(normed[...], full[0][:, i * ret : (i + 1) * ret])
        proj[i] = (piece * scale[:, i * ret : (i + 1) * ret]).astype(BF)

    r = lax.broadcasted_iota(jnp.int32, (ret, ret), 0)
    c = lax.broadcasted_iota(jnp.int32, (ret, ret), 1)
    odd = lax.rem(c, 2) == 1
    swap = jnp.where((r == c - 1) & odd, 1.0, jnp.where((r == c + 1) & ~odd, -1.0, 0.0)).astype(BF)
    same = jnp.where(r // head == c // head, 1.0 / head, 0.0).astype(F32)

    def turn(field):
        return field.astype(F32) * cos_t[...] + nn(field, swap) * sin_t[...]

    rot_q = turn(proj[0])
    rot_k = (turn(proj[1]) * head ** (-0.5)).astype(BF)
    vals = proj[2]
    rows = lax.broadcasted_iota(jnp.int32, (length, length), 0)
    cols = lax.broadcasted_iota(jnp.int32, (length, length), 1)
    dist = (rows - cols).astype(F32)
    lane = lax.broadcasted_iota(jnp.int32, (length, ret), 1) // head
    total = jnp.zeros((length, ret), F32)
    for h in range(heads):
        q_h = jnp.where(lane == h, rot_q, 0.0).astype(BF)
        decay = jnp.where(dist >= 0.0, jnp.exp(-forget[h] * jnp.maximum(dist, 0.0)), 0.0)
        inner = (nt(q_h, rot_k) * decay).astype(BF)
        total = jnp.where(lane == h, nn(inner, vals), total)
    mean = lax.dot_general(
        total * total, same, (((1,), (0,)), ((), ())), precision=lax.Precision.HIGHEST, preferred_element_type=F32
    )
    gate = proj[3].astype(F32)
    mixed[...] = (gate / (1.0 + jnp.exp(-gate)) * (total * lax.rsqrt(mean + 0.01))).astype(BF)

    finish(1)
    for t in range(n_tp):
        mix_p[t] = nt(mixed[...], full[1][t * width : (t + 1) * width, :]).astype(BF)
    tp_scatter(1, mix_p, mix_r)
    relay(ups[0])
    after = (tok[...].astype(F32) + tp_sum(1, mix_p, mix_r) * out_scale).astype(BF)
    am_g[tp] = after
    tp_gather(2, am_g.at[tp], am_g)
    x_own(downs[0])
    relay(ups[1])
    tp_wait(2, am_g)
    norm(am_g, 1)

    chain = ups + downs
    for w in downs[1:]:
        x_own(w)
    for i, w in enumerate(chain):
        if i + 1 < len(chain) and i + 1 > 1:
            relay(chain[i + 1])
        finish(w)
        if i < n_ch:
            size = full[w].shape[1]
            step = size // max(1, size // 256)

            def up_tile(j, carry, w=w, i=i, size=size, step=step):
                here = pl.ds(pl.multiple_of(j * step, step), step)
                u = nn(normed[...], full[w][:, here])
                s = scale_row[:, pl.ds(pl.multiple_of(up_at + i * size + j * step, 128), step)]
                u = jnp.maximum(u * s, 0.0)
                hidden[i, :, here] = (u * u).astype(BF)
                return carry

            lax.fori_loop(0, size // step, up_tile, 0)
        else:
            k = i - n_ch

            def down_tile(t, carry, w=w, k=k):
                part = nt(hidden[k], full[w][pl.ds(pl.multiple_of(t * width, width), width), :])
                if k:
                    part = part + acc[t]
                if k < n_ch - 1:
                    acc[t] = part
                else:
                    mlp_p[t] = part.astype(BF)
                return carry

            lax.fori_loop(0, n_tp, down_tile, 0)
    tp_scatter(3, mlp_p, mlp_r)
    out_ref[...] = (am_g[tp].astype(F32) + tp_sum(3, mlp_p, mlp_r) * down_scale).astype(BF)
    for copy in pending:
        copy.wait_send()


def tables(length, head, heads):
    half = head // 2
    inverse = 1.0 / 10000.0 ** np.linspace(0.0, 1.0, half)
    angle = np.arange(length)[:, None] * inverse.astype(np.float32).astype(np.float64)[None, :]
    spread = lambda a: np.tile(np.repeat(a, 2, axis=1), (1, heads)).astype(np.float32)
    return spread(np.cos(angle)), spread(np.sin(angle))


def solution(mesh):
    n_fs, n_tp = mesh.shape["fs"], mesh.shape["tp"]
    heights = [getattr(d, "coords", (0, 0, i))[2] for i, d in enumerate(mesh.devices[:, 0])]
    X = heights.count(heights[0])
    if n_fs % X:
        X = 1
    Z = n_fs // X

    def on_device(tokens, mix_gain, mlp_gain, wq, wk, wv, wg, wo, wu, wd, sq, sk, sv, sg, so, su, sd, forget):
        width, length = tokens.shape
        D = width * n_tp
        ret = wq.shape[1]
        heads = forget.shape[0]
        ff = wu.shape[1]
        n_ch = 4 if ff % 512 == 0 else 1
        chunk = ff // n_ch
        me = lax.axis_index("fs")

        def spot(s):
            wide = jnp.tile(s, n_fs)
            return jnp.where(jnp.arange(wide.shape[0]) // s.shape[0] == me, wide, 0.0)

        scales = jnp.concatenate([spot(s) for s in (sq, sk, sv, sg, so, sd, su)])[None, :]
        gains = jnp.stack([mix_gain, mlp_gain])
        cos_t, sin_t = tables(length, ret // heads, heads)
        own = [jnp.concatenate([w.astype(BF) for w in (wq, wk, wv, wg)], axis=1), wo.astype(BF).T]
        own += [wu[:, i * chunk : (i + 1) * chunk].astype(BF) for i in range(n_ch)]
        own += [wd[i * chunk : (i + 1) * chunk].astype(BF).T for i in range(n_ch)]
        n_w = len(own)
        vm = pl.BlockSpec(memory_space=pltpu.VMEM)
        block = (n_tp, length, width)
        dma = pltpu.SemaphoreType.DMA
        scratch = [pltpu.VMEM((n_fs * w.shape[0], w.shape[1]), BF) for w in own]
        scratch += [
            pltpu.VMEM((n_fs,) + scales.shape, F32),
            pltpu.VMEM(block, BF),
            pltpu.VMEM(block, BF),
            pltpu.VMEM((n_tp - 1,) + block[1:], BF),
            pltpu.VMEM(block, BF),
            pltpu.VMEM(block, BF),
            pltpu.VMEM((n_tp - 1,) + block[1:], BF),
            pltpu.VMEM((length, D), BF),
            pltpu.VMEM((4, length, ret), BF),
            pltpu.VMEM((length, ret), BF),
            pltpu.VMEM((n_ch, length, chunk), BF),
            pltpu.VMEM(block, F32),
            pltpu.VMEM(scales.shape, F32),
            dma((n_w + 2,)),
            dma((n_w + 1, Z - 1)),
            dma((n_w + 1, Z - 1)),
            dma((n_w + 1, Z, X - 1)),
            dma((n_w + 1, Z, X - 1)),
            dma((4, n_tp - 1)),
            dma((4, n_tp - 1)),
        ]
        out = pl.pallas_call(
            functools.partial(kernel, (Z, X, n_tp, n_ch, heads)),
            out_shape=jax.ShapeDtypeStruct((length, width), BF),
            in_specs=[vm] * 5 + [pl.BlockSpec(memory_space=pltpu.SMEM)] + [vm] * n_w,
            out_specs=vm,
            scratch_shapes=scratch,
            compiler_params=pltpu.CompilerParams(
                collective_id=0, has_side_effects=True, vmem_limit_bytes=60 * 2**20
            ),
            name="layer",
        )(tokens.T, gains, scales, jnp.asarray(cos_t), jnp.asarray(sin_t), forget, *own)
        return out.T

    cut = P(("tp", "fs"))
    rows, cols = P("fs", "tp"), P("tp", "fs")
    in_specs = (cols, P(), P(), rows, rows, rows, rows, cols, rows, cols) + (cut,) * 7 + (P("tp"),)
    return jax.shard_map(on_device, mesh=mesh, in_specs=in_specs, out_specs=cols, check_vma=False)
```

```python
import functools

import jax
import jax.numpy as jnp
import numpy as np
from jax import lax
from jax.experimental import pallas as pl
from jax.experimental.pallas import tpu as pltpu
from jax.sharding import PartitionSpec as P

MESH = pl.DeviceIdType.MESH
BF = jnp.bfloat16
F32 = jnp.float32


def nn(a, b):
    return lax.dot_general(a, b, (((1,), (0,)), ((), ())), preferred_element_type=F32)


def nt(a, b):
    return lax.dot_general(a, b, (((1,), (1,)), ((), ())), preferred_element_type=F32)


def kernel(cfg, *refs):
    Z, X, Y, C, heads = cfg
    n_tp = Y * C
    n_w = 4
    tok, gains, scales, cos_t, sin_t, forget = refs[:6]
    own = refs[6 : 6 + n_w]
    out_ref = refs[6 + n_w]
    rest = refs[7 + n_w :]
    full = rest[:n_w]
    (scale_g, scale_row, tok_g, seqs, parts, core_in, y_out, y_in, z_out, z_in, normed, proj, mixed, hidden,
     local_sem, zs, zr, xs, xr, ts, tr, azs, azr, ays, ayr, acs, acr, rcs, rcr, rys, ryr, rzs, rzr) = rest[n_w:]
    me = lax.axis_index("fs")
    tp = lax.axis_index("tp")
    z = me // X
    x = lax.rem(me, X)
    y = tp // C
    core = lax.rem(tp, C)
    length, width = tok.shape
    ret = mixed.shape[1]
    head = ret // heads

    def at_z(o):
        return lax.rem(z + o, Z) * X + x

    def at_x(o):
        return z * X + lax.rem(x + o, X)

    def at_tp(o):
        return lax.rem(tp + o, n_tp)

    def at_y(o):
        return lax.rem(y + o, Y) * C + core

    def at_core(o):
        return y * C + lax.rem(core + o, C)

    barrier = pltpu.get_barrier_semaphore()
    for o in range(1, Z):
        pl.semaphore_signal(barrier, inc=1, device_id={"fs": at_z(o)}, device_id_type=MESH)
    for o in range(1, X):
        pl.semaphore_signal(barrier, inc=1, device_id={"fs": at_x(o)}, device_id_type=MESH)
    for o in range(1, n_tp):
        pl.semaphore_signal(barrier, inc=1, device_id={"tp": at_tp(o)}, device_id_type=MESH)
    pl.semaphore_wait(barrier, Z - 1 + X - 1 + n_tp - 1)

    pending = []

    def remote(src, dst, ss, rs, where):
        return pltpu.make_async_remote_copy(
            src_ref=src, dst_ref=dst, send_sem=ss, recv_sem=rs, device_id=where, device_id_type=MESH
        )

    def send(*parts_of):
        copy = remote(*parts_of)
        copy.start()
        pending.append(copy)

    def place(w, owner):
        if w == n_w:
            return scale_g.at[owner]
        rows = own[w].shape[-2]
        return full[w].at[pl.ds(pl.multiple_of(owner * rows, rows), rows)]

    def mine(w, o):
        if w == n_w:
            return scales
        return own[w].at[lax.rem(z + o, Z)] if w >= 2 else own[w]

    def z_send(w):
        for o in range(1, Z):
            send(mine(w, o), place(w, me), zs.at[w, o - 1], zr.at[w, o - 1], {"fs": at_z(o)})

    def x_own(w):
        for o in range(1, X):
            send(mine(w, 0), place(w, me), xs.at[w, 0, o - 1], xr.at[w, 0, o - 1], {"fs": at_x(o)})

    def relay(w):
        for k in range(1, Z):
            piece = place(w, at_z(Z - k))
            remote(piece, piece, zs.at[w, k - 1], zr.at[w, k - 1], {"fs": at_z(k)}).wait_recv()
            for o in range(1, X):
                send(piece, piece, xs.at[w, k, o - 1], xr.at[w, k, o - 1], {"fs": at_x(o)})

    def finish(w):
        for k in range(Z):
            for o in range(1, X):
                owner = lax.rem(z + Z - k, Z) * X + lax.rem(x + X - o, X)
                piece = place(w, owner)
                remote(piece, piece, xs.at[w, k, o - 1], xr.at[w, k, o - 1], {"fs": at_x(o)}).wait_recv()

    def store_parts(k, t, value):
        parts[k, t % C, t // C] = value.astype(BF)

    def reduce_start(k):
        for o in range(1, C):
            send(parts.at[k, lax.rem(core + o, C)], core_in.at[k, o - 1], rcs.at[k, o - 1], rcr.at[k, o - 1],
                 {"tp": at_core(o)})

    def reduce_core(k):
        for o in range(1, C):
            slot = core_in.at[k, o - 1]
            remote(slot, slot, rcs.at[k, o - 1], rcr.at[k, o - 1], {"tp": at_core(o)}).wait_recv()
        for j in range(Y):
            value = parts[k, core, j].astype(F32)
            for o in range(1, C):
                value += core_in[k, o - 1, j].astype(F32)
            y_out[k, j] = value.astype(BF)
        for j in range(1, Y):
            send(y_out.at[k, lax.rem(y + j, Y)], y_in.at[k, j - 1], rys.at[k, j - 1], ryr.at[k, j - 1],
                 {"tp": at_y(j)})

    def reduce_y(k):
        value = y_out[k, y].astype(F32)
        for j in range(1, Y):
            slot = y_in.at[k, j - 1]
            remote(slot, slot, rys.at[k, j - 1], ryr.at[k, j - 1], {"tp": at_y(j)}).wait_recv()
            value += y_in[k, j - 1].astype(F32)
        return value

    def norm(block, row):
        square = jnp.zeros((length, 1), F32)
        for t in range(n_tp):
            v = block(t)[...].astype(F32)
            square += jnp.sum(v * v, axis=-1, keepdims=True)
        factor = lax.rsqrt(square / (width * n_tp) + 1e-6)
        for t in range(n_tp):
            cols = slice(t * width, (t + 1) * width)
            normed[:, cols] = (block(t)[...].astype(F32) * factor * gains[row : row + 1, cols]).astype(BF)

    for o in range(1, n_tp):
        send(tok, tok_g.at[tp], ts.at[o - 1], tr.at[o - 1], {"tp": at_tp(o)})
    for w in (n_w, 0, 1):
        z_send(w)
        x_own(w)
    z_send(2)
    z_send(3)
    locals_ = [pltpu.make_async_copy(mine(w, 0), place(w, me), local_sem.at[w]) for w in range(n_w + 1)]
    locals_.append(pltpu.make_async_copy(tok, tok_g.at[tp], local_sem.at[n_w + 1]))
    for copy in locals_:
        copy.start()
    for copy in locals_:
        copy.wait()
    for o in range(1, n_tp):
        slot = tok_g.at[at_tp(n_tp - o)]
        remote(slot, slot, ts.at[o - 1], tr.at[o - 1], {"tp": at_tp(o)}).wait_recv()
    norm(lambda t: tok_g.at[t], 0)

    relay(n_w)
    relay(0)
    relay(1)
    x_own(2)
    x_own(3)
    finish(n_w)
    finish(0)
    scale = jnp.sum(scale_g[...], axis=0)
    scale_row[...] = scale
    at = 4 * ret
    out_scale = scale[:, at : at + width]
    down_scale = scale[:, at + width : at + 2 * width]
    up_at = at + 2 * width

    for i in range(4):
        piece = nn(normed[...], full[0][:, i * ret : (i + 1) * ret])
        proj[i] = (piece * scale[:, i * ret : (i + 1) * ret]).astype(BF)

    r = lax.broadcasted_iota(jnp.int32, (ret, ret), 0)
    c = lax.broadcasted_iota(jnp.int32, (ret, ret), 1)
    odd = lax.rem(c, 2) == 1
    swap = jnp.where((r == c - 1) & odd, 1.0, jnp.where((r == c + 1) & ~odd, -1.0, 0.0)).astype(BF)
    same = jnp.where(r // head == c // head, 1.0 / head, 0.0).astype(F32)

    def turn(field):
        return field.astype(F32) * cos_t[...] + nn(field, swap) * sin_t[...]

    rot_q = turn(proj[0])
    rot_k = (turn(proj[1]) * head ** (-0.5)).astype(BF)
    vals = proj[2]
    rows = lax.broadcasted_iota(jnp.int32, (length, length), 0)
    cols = lax.broadcasted_iota(jnp.int32, (length, length), 1)
    dist = (rows - cols).astype(F32)
    lane = lax.broadcasted_iota(jnp.int32, (length, ret), 1) // head
    total = jnp.zeros((length, ret), F32)
    for h in range(heads):
        q_h = jnp.where(lane == h, rot_q, 0.0).astype(BF)
        decay = jnp.where(dist >= 0.0, jnp.exp(-forget[h] * jnp.maximum(dist, 0.0)), 0.0)
        inner = (nt(q_h, rot_k) * decay).astype(BF)
        total = jnp.where(lane == h, nn(inner, vals), total)
    mean = lax.dot_general(
        total * total, same, (((1,), (0,)), ((), ())), precision=lax.Precision.HIGHEST, preferred_element_type=F32
    )
    gate = proj[3].astype(F32)
    mixed[...] = (gate / (1.0 + jnp.exp(-gate)) * (total * lax.rsqrt(mean + 0.01))).astype(BF)

    finish(1)
    for t in range(n_tp):
        store_parts(Z, t, nt(mixed[...], full[1][t * width : (t + 1) * width, :]))
    reduce_start(Z)
    reduce_core(Z)
    relay(2)
    after = (tok[...].astype(F32) + reduce_y(Z) * out_scale).astype(BF)
    seqs[0, tp] = after

    for k in range(1, Z):
        send(seqs.at[0, tp], seqs.at[k, tp], azs.at[k - 1], azr.at[k - 1], {"fs": at_z(k)})

    def collect_z(k):
        slot = seqs.at[k, tp]
        if k:
            remote(slot, slot, azs.at[k - 1], azr.at[k - 1], {"fs": at_z(k)}).wait_recv()
        for j in range(1, Y):
            send(slot, slot, ays.at[k, j - 1], ayr.at[k, j - 1], {"tp": at_y(j)})
        for o in range(1, C):
            send(slot, slot, acs.at[k, 0, o - 1], acr.at[k, 0, o - 1], {"tp": at_core(o)})

    def collect_y(k):
        for j in range(1, Y):
            slot = seqs.at[k, at_y(Y - j)]
            remote(slot, slot, ays.at[k, j - 1], ayr.at[k, j - 1], {"tp": at_y(j)}).wait_recv()
            for o in range(1, C):
                send(slot, slot, acs.at[k, j, o - 1], acr.at[k, j, o - 1], {"tp": at_core(o)})

    def feed(k):
        for j in range(Y):
            for o in range(1, C):
                slot = seqs.at[k, lax.rem(y + Y - j, Y) * C + lax.rem(core + C - o, C)]
                remote(slot, slot, acs.at[k, j, o - 1], acr.at[k, j, o - 1], {"tp": at_core(o)}).wait_recv()
        norm(lambda t: seqs.at[k, t], 1)
        if k == 0:
            finish(2)
        chunk = hidden.shape[1]
        s = scale_row[:, pl.ds(pl.multiple_of(up_at + z * chunk, 128), chunk)]
        u = jnp.maximum(nn(normed[...], full[2][...]) * s, 0.0)
        hidden[...] = (u * u).astype(BF)
        if k == 0:
            finish(3)
        for t in range(n_tp):
            store_parts(k, t, nt(hidden[...], full[3][t * width : (t + 1) * width, :]))
        reduce_start(k)

    def give_z(k):
        value = reduce_y(k)
        z_out[k] = value.astype(BF)
        if k:
            send(z_out.at[k], z_in.at[k - 1], rzs.at[k - 1], rzr.at[k - 1], {"fs": at_z(Z - k)})

    collect_z(0)
    relay(3)
    for i in range(Z + 3):
        if 1 <= i + 1 < Z:
            collect_z(i + 1)
        if i < Z:
            collect_y(i)
        if 0 <= i - 1 < Z:
            reduce_core(i - 1)
        if 0 <= i - 2 < Z:
            give_z(i - 2)
        if i < Z:
            feed(i)
    mlp_total = z_out[0].astype(F32)
    for k in range(1, Z):
        slot = z_in.at[k - 1]
        remote(slot, slot, rzs.at[k - 1], rzr.at[k - 1], {"fs": at_z(k)}).wait_recv()
        mlp_total += z_in[k - 1].astype(F32)
    out_ref[...] = (seqs[0, tp].astype(F32) + mlp_total * down_scale).astype(BF)
    for copy in pending:
        copy.wait_send()


def tables(length, head, heads):
    half = head // 2
    inverse = 1.0 / 10000.0 ** np.linspace(0.0, 1.0, half)
    angle = np.arange(length)[:, None] * inverse.astype(np.float32).astype(np.float64)[None, :]
    spread = lambda a: np.tile(np.repeat(a, 2, axis=1), (1, heads)).astype(np.float32)
    return spread(np.cos(angle)), spread(np.sin(angle))


def solution(mesh):
    n_fs, n_tp = mesh.shape["fs"], mesh.shape["tp"]
    heights = [getattr(d, "coords", (0, 0, i))[2] for i, d in enumerate(mesh.devices[:, 0])]
    X = heights.count(heights[0])
    if n_fs % X:
        X = 1
    Z = n_fs // X
    cores = [getattr(d, "core_on_chip", 0) for d in mesh.devices[0]]
    C = len(set(cores))
    if n_tp % C:
        C = 1
    Y = n_tp // C

    def on_device(tokens, mix_gain, mlp_gain, wq, wk, wv, wg, wo, wu, wd, sq, sk, sv, sg, so, su, sd, forget):
        width, length = tokens.shape
        D = width * n_tp
        ret = wq.shape[1]
        heads = forget.shape[0]
        ff = wu.shape[1]
        chunk = ff // Z
        me = lax.axis_index("fs")

        def spot(s):
            wide = jnp.tile(s, n_fs)
            return jnp.where(jnp.arange(wide.shape[0]) // s.shape[0] == me, wide, 0.0)

        scales = jnp.concatenate([spot(s) for s in (sq, sk, sv, sg, so, sd, su)])[None, :]
        gains = jnp.stack([mix_gain, mlp_gain])
        cos_t, sin_t = tables(length, ret // heads, heads)
        own = [jnp.concatenate([w.astype(BF) for w in (wq, wk, wv, wg)], axis=1), wo.astype(BF).T]
        own.append(wu.astype(BF).reshape(-1, Z, chunk).transpose(1, 0, 2))
        own.append(wd.astype(BF).reshape(Z, chunk, -1).transpose(0, 2, 1))
        n_w = len(own)
        vm = pl.BlockSpec(memory_space=pltpu.VMEM)
        dma = pltpu.SemaphoreType.DMA
        tile = (length, width)
        scratch = [pltpu.VMEM((n_fs * w.shape[-2], w.shape[-1]), BF) for w in own]
        scratch += [
            pltpu.VMEM((n_fs,) + scales.shape, F32),
            pltpu.VMEM(scales.shape, F32),
            pltpu.VMEM((n_tp,) + tile, BF),
            pltpu.VMEM((Z, n_tp) + tile, BF),
            pltpu.VMEM((Z + 1, C, Y) + tile, BF),
            pltpu.VMEM((Z + 1, C - 1, Y) + tile, BF),
            pltpu.VMEM((Z + 1, Y) + tile, BF),
            pltpu.VMEM((Z + 1, Y - 1) + tile, BF),
            pltpu.VMEM((Z,) + tile, BF),
            pltpu.VMEM((Z - 1,) + tile, BF),
            pltpu.VMEM((length, D), BF),
            pltpu.VMEM((4, length, ret), BF),
            pltpu.VMEM((length, ret), BF),
            pltpu.VMEM((length, chunk), BF),
            dma((n_w + 2,)),
        ]
        for shape in [(n_w + 1, Z - 1), (n_w + 1, Z, X - 1), (n_tp - 1,), (Z - 1,), (Z, Y - 1), (Z, Y, C - 1),
                      (Z + 1, C - 1), (Z + 1, Y - 1), (Z - 1,)]:
            scratch += [dma(shape), dma(shape)]
        out = pl.pallas_call(
            functools.partial(kernel, (Z, X, Y, C, heads)),
            out_shape=jax.ShapeDtypeStruct((length, width), BF),
            in_specs=[vm] * 5 + [pl.BlockSpec(memory_space=pltpu.SMEM)] + [vm] * n_w,
            out_specs=vm,
            scratch_shapes=scratch,
            compiler_params=pltpu.CompilerParams(
                collective_id=0, has_side_effects=True, vmem_limit_bytes=60 * 2**20
            ),
            name="layer",
        )(tokens.T, gains, scales, jnp.asarray(cos_t), jnp.asarray(sin_t), forget, *own)
        return out.T

    cut = P(("tp", "fs"))
    rows, cols = P("fs", "tp"), P("tp", "fs")
    in_specs = (cols, P(), P(), rows, rows, rows, rows, cols, rows, cols) + (cut,) * 7 + (P("tp"),)
    return jax.shard_map(on_device, mesh=mesh, in_specs=in_specs, out_specs=cols, check_vma=False)
```

```python
import functools

import jax
import jax.numpy as jnp
import numpy as np
from jax import lax
from jax.experimental import pallas as pl
from jax.experimental.pallas import tpu as pltpu
from jax.sharding import PartitionSpec as P

MESH = pl.DeviceIdType.MESH
BF = jnp.bfloat16
F32 = jnp.float32


def nn(a, b):
    return lax.dot_general(a, b, (((1,), (0,)), ((), ())), preferred_element_type=F32)


def nt(a, b):
    return lax.dot_general(a, b, (((1,), (1,)), ((), ())), preferred_element_type=F32)


def kernel(cfg, *refs):
    Z, X, Y, C, G, heads = cfg
    n_tp = Y * C
    n_w = 4
    tok, gains, scales, cos_t, sin_t, forget = refs[:6]
    own = refs[6 : 6 + n_w]
    out_ref = refs[6 + n_w]
    rest = refs[7 + n_w :]
    full = rest[:n_w]
    (scale_g, scale_row, tok_g, seqs, parts, core_in, y_out, y_in, z_out, z_in, normed, proj, mixed, hidden,
     local_sem, zs, zr, xs, xr, ts, tr, azs, azr, ays, ayr, acs, acr, rcs, rcr, rys, ryr, rzs, rzr) = rest[n_w:]
    me = lax.axis_index("fs")
    tp = lax.axis_index("tp")
    z = me // X
    x = lax.rem(me, X)
    y = tp // C
    core = lax.rem(tp, C)
    length, width = tok.shape
    ret = mixed.shape[1]
    head = ret // heads

    def at_z(o):
        return lax.rem(z + o, Z) * X + x

    def at_g(o):
        return (z // G * G + lax.rem(z + o, G)) * X + x

    def at_x(o):
        return z * X + lax.rem(x + o, X)

    def at_tp(o):
        return lax.rem(tp + o, n_tp)

    def at_y(o):
        return lax.rem(y + o, Y) * C + core

    def at_core(o):
        return y * C + lax.rem(core + o, C)

    barrier = pltpu.get_barrier_semaphore()
    for o in range(1, Z):
        pl.semaphore_signal(barrier, inc=1, device_id={"fs": at_z(o)}, device_id_type=MESH)
    for o in range(1, X):
        pl.semaphore_signal(barrier, inc=1, device_id={"fs": at_x(o)}, device_id_type=MESH)
    for o in range(1, n_tp):
        pl.semaphore_signal(barrier, inc=1, device_id={"tp": at_tp(o)}, device_id_type=MESH)
    pl.semaphore_wait(barrier, Z - 1 + X - 1 + n_tp - 1)

    pending = []

    def remote(src, dst, ss, rs, where):
        return pltpu.make_async_remote_copy(
            src_ref=src, dst_ref=dst, send_sem=ss, recv_sem=rs, device_id=where, device_id_type=MESH
        )

    def send(*parts_of):
        copy = remote(*parts_of)
        copy.start()
        pending.append(copy)

    def place(w, owner):
        if w == n_w:
            return scale_g.at[owner]
        rows = own[w].shape[-2]
        return full[w].at[pl.ds(pl.multiple_of(owner * rows, rows), rows)]

    def mine(w, o):
        if w == n_w:
            return scales
        return own[w].at[lax.rem(z + o, G)] if w >= 2 else own[w]

    def z_send(w):
        for o in range(1, Z):
            send(mine(w, o), place(w, me), zs.at[w, o - 1], zr.at[w, o - 1], {"fs": at_z(o)})

    def x_own(w):
        for o in range(1, X):
            send(mine(w, 0), place(w, me), xs.at[w, 0, o - 1], xr.at[w, 0, o - 1], {"fs": at_x(o)})

    def relay(w):
        for k in range(1, Z):
            piece = place(w, at_z(Z - k))
            remote(piece, piece, zs.at[w, k - 1], zr.at[w, k - 1], {"fs": at_z(k)}).wait_recv()
            for o in range(1, X):
                send(piece, piece, xs.at[w, k, o - 1], xr.at[w, k, o - 1], {"fs": at_x(o)})

    def finish(w):
        for k in range(Z):
            for o in range(1, X):
                owner = lax.rem(z + Z - k, Z) * X + lax.rem(x + X - o, X)
                piece = place(w, owner)
                remote(piece, piece, xs.at[w, k, o - 1], xr.at[w, k, o - 1], {"fs": at_x(o)}).wait_recv()

    def store_parts(k, t, value):
        parts[k, t % C, t // C] = value.astype(BF)

    def reduce_start(k):
        for o in range(1, C):
            send(parts.at[k, lax.rem(core + o, C)], core_in.at[k, o - 1], rcs.at[k, o - 1], rcr.at[k, o - 1],
                 {"tp": at_core(o)})

    def reduce_core(k):
        for o in range(1, C):
            slot = core_in.at[k, o - 1]
            remote(slot, slot, rcs.at[k, o - 1], rcr.at[k, o - 1], {"tp": at_core(o)}).wait_recv()
        for j in range(Y):
            value = parts[k, core, j].astype(F32)
            for o in range(1, C):
                value += core_in[k, o - 1, j].astype(F32)
            y_out[k, j] = value.astype(BF)
        for j in range(1, Y):
            send(y_out.at[k, lax.rem(y + j, Y)], y_in.at[k, j - 1], rys.at[k, j - 1], ryr.at[k, j - 1],
                 {"tp": at_y(j)})

    def reduce_y(k):
        value = y_out[k, y].astype(F32)
        for j in range(1, Y):
            slot = y_in.at[k, j - 1]
            remote(slot, slot, rys.at[k, j - 1], ryr.at[k, j - 1], {"tp": at_y(j)}).wait_recv()
            value += y_in[k, j - 1].astype(F32)
        return value

    def norm(block, row):
        square = jnp.zeros((length, 1), F32)
        for t in range(n_tp):
            v = block(t)[...].astype(F32)
            square += jnp.sum(v * v, axis=-1, keepdims=True)
        factor = lax.rsqrt(square / (width * n_tp) + 1e-6)
        for t in range(n_tp):
            cols = slice(t * width, (t + 1) * width)
            normed[:, cols] = (block(t)[...].astype(F32) * factor * gains[row : row + 1, cols]).astype(BF)

    for o in range(1, n_tp):
        send(tok, tok_g.at[tp], ts.at[o - 1], tr.at[o - 1], {"tp": at_tp(o)})
    for w in (n_w, 0, 1):
        z_send(w)
        x_own(w)
    z_send(2)
    locals_ = [pltpu.make_async_copy(mine(w, 0), place(w, me), local_sem.at[w]) for w in range(n_w + 1)]
    locals_.append(pltpu.make_async_copy(tok, tok_g.at[tp], local_sem.at[n_w + 1]))
    for copy in locals_:
        copy.start()
    for copy in locals_:
        copy.wait()
    for o in range(1, n_tp):
        slot = tok_g.at[at_tp(n_tp - o)]
        remote(slot, slot, ts.at[o - 1], tr.at[o - 1], {"tp": at_tp(o)}).wait_recv()
    norm(lambda t: tok_g.at[t], 0)

    relay(n_w)
    relay(0)
    relay(1)
    x_own(2)
    x_own(3)
    finish(n_w)
    finish(0)
    scale = jnp.sum(scale_g[...], axis=0)
    scale_row[...] = scale
    at = 4 * ret
    out_scale = scale[:, at : at + width]
    down_scale = scale[:, at + width : at + 2 * width]
    up_at = at + 2 * width

    for i in range(4):
        piece = nn(normed[...], full[0][:, i * ret : (i + 1) * ret])
        proj[i] = (piece * scale[:, i * ret : (i + 1) * ret]).astype(BF)

    r = lax.broadcasted_iota(jnp.int32, (ret, ret), 0)
    c = lax.broadcasted_iota(jnp.int32, (ret, ret), 1)
    odd = lax.rem(c, 2) == 1
    swap = jnp.where((r == c - 1) & odd, 1.0, jnp.where((r == c + 1) & ~odd, -1.0, 0.0)).astype(BF)
    same = jnp.where(r // head == c // head, 1.0 / head, 0.0).astype(F32)

    def turn(field):
        return field.astype(F32) * cos_t[...] + nn(field, swap) * sin_t[...]

    rot_q = turn(proj[0])
    rot_k = (turn(proj[1]) * head ** (-0.5)).astype(BF)
    vals = proj[2]
    rows = lax.broadcasted_iota(jnp.int32, (length, length), 0)
    cols = lax.broadcasted_iota(jnp.int32, (length, length), 1)
    dist = (rows - cols).astype(F32)
    lane = lax.broadcasted_iota(jnp.int32, (length, ret), 1) // head
    total = jnp.zeros((length, ret), F32)
    for h in range(heads):
        q_h = jnp.where(lane == h, rot_q, 0.0).astype(BF)
        decay = jnp.where(dist >= 0.0, jnp.exp(-forget[h] * jnp.maximum(dist, 0.0)), 0.0)
        inner = (nt(q_h, rot_k) * decay).astype(BF)
        total = jnp.where(lane == h, nn(inner, vals), total)
    mean = lax.dot_general(
        total * total, same, (((1,), (0,)), ((), ())), precision=lax.Precision.HIGHEST, preferred_element_type=F32
    )
    gate = proj[3].astype(F32)
    mixed[...] = (gate / (1.0 + jnp.exp(-gate)) * (total * lax.rsqrt(mean + 0.01))).astype(BF)

    finish(1)
    for t in range(n_tp):
        store_parts(G, t, nt(mixed[...], full[1][t * width : (t + 1) * width, :]))
    reduce_start(G)
    reduce_core(G)
    after = (tok[...].astype(F32) + reduce_y(G) * out_scale).astype(BF)
    seqs[0, tp] = after

    for k in range(1, G):
        send(seqs.at[0, tp], seqs.at[k, tp], azs.at[k - 1], azr.at[k - 1], {"fs": at_g(k)})
    z_send(3)

    def collect_z(k):
        slot = seqs.at[k, tp]
        if k:
            remote(slot, slot, azs.at[k - 1], azr.at[k - 1], {"fs": at_g(k)}).wait_recv()
        for j in range(1, Y):
            send(slot, slot, ays.at[k, j - 1], ayr.at[k, j - 1], {"tp": at_y(j)})
        for o in range(1, C):
            send(slot, slot, acs.at[k, 0, o - 1], acr.at[k, 0, o - 1], {"tp": at_core(o)})

    def collect_y(k):
        for j in range(1, Y):
            slot = seqs.at[k, at_y(Y - j)]
            remote(slot, slot, ays.at[k, j - 1], ayr.at[k, j - 1], {"tp": at_y(j)}).wait_recv()
            for o in range(1, C):
                send(slot, slot, acs.at[k, j, o - 1], acr.at[k, j, o - 1], {"tp": at_core(o)})

    def feed(k):
        for j in range(Y):
            for o in range(1, C):
                slot = seqs.at[k, lax.rem(y + Y - j, Y) * C + lax.rem(core + C - o, C)]
                remote(slot, slot, acs.at[k, j, o - 1], acr.at[k, j, o - 1], {"tp": at_core(o)}).wait_recv()
        norm(lambda t: seqs.at[k, t], 1)

    def expand(k):
        chunk = hidden.shape[2]
        step = 256 if chunk % 256 == 0 else chunk

        def tile(i, carry):
            here = pl.ds(pl.multiple_of(i * step, step), step)
            s = scale_row[:, pl.ds(pl.multiple_of(up_at + lax.rem(z, G) * chunk + i * step, 128), step)]
            u = jnp.maximum(nn(normed[...], full[2][:, here]) * s, 0.0)
            hidden[k, :, here] = (u * u).astype(BF)
            return carry

        lax.fori_loop(0, chunk // step, tile, 0)

    def shrink(k):
        for t in range(n_tp):
            store_parts(k, t, nt(hidden[k], full[3][t * width : (t + 1) * width, :]))
        reduce_start(k)

    def give_z(k):
        value = reduce_y(k)
        z_out[k] = value.astype(BF)
        if k:
            send(z_out.at[k], z_in.at[k - 1], rzs.at[k - 1], rzr.at[k - 1], {"fs": at_g(G - k)})

    collect_z(0)
    relay(2)
    for k in range(1, G):
        collect_z(k)
    collect_y(0)
    feed(0)
    finish(2)
    expand(0)
    for k in range(1, G):
        collect_y(k)
        feed(k)
        expand(k)
    relay(3)
    finish(3)
    order = list(range(1, G)) + [0]
    for k in order:
        shrink(k)
    for k in order:
        reduce_core(k)
    for k in order:
        give_z(k)
    mlp_total = z_out[0].astype(F32)
    for k in range(1, G):
        slot = z_in.at[k - 1]
        remote(slot, slot, rzs.at[k - 1], rzr.at[k - 1], {"fs": at_g(k)}).wait_recv()
        mlp_total += z_in[k - 1].astype(F32)
    out_ref[...] = (seqs[0, tp].astype(F32) + mlp_total * down_scale).astype(BF)
    for copy in pending:
        copy.wait_send()


def tables(length, head, heads):
    half = head // 2
    inverse = 1.0 / 10000.0 ** np.linspace(0.0, 1.0, half)
    angle = np.arange(length)[:, None] * inverse.astype(np.float32).astype(np.float64)[None, :]
    spread = lambda a: np.tile(np.repeat(a, 2, axis=1), (1, heads)).astype(np.float32)
    return spread(np.cos(angle)), spread(np.sin(angle))


def solution(mesh):
    n_fs, n_tp = mesh.shape["fs"], mesh.shape["tp"]
    heights = [getattr(d, "coords", (0, 0, i))[2] for i, d in enumerate(mesh.devices[:, 0])]
    X = heights.count(heights[0])
    if n_fs % X:
        X = 1
    Z = n_fs // X
    cores = [getattr(d, "core_on_chip", 0) for d in mesh.devices[0]]
    C = len(set(cores))
    if n_tp % C:
        C = 1
    Y = n_tp // C
    G = 2 if Z % 2 == 0 else Z

    def on_device(tokens, mix_gain, mlp_gain, wq, wk, wv, wg, wo, wu, wd, sq, sk, sv, sg, so, su, sd, forget):
        width, length = tokens.shape
        D = width * n_tp
        ret = wq.shape[1]
        heads = forget.shape[0]
        ff = wu.shape[1]
        chunk = ff // G
        me = lax.axis_index("fs")

        def spot(s):
            wide = jnp.tile(s, n_fs)
            return jnp.where(jnp.arange(wide.shape[0]) // s.shape[0] == me, wide, 0.0)

        scales = jnp.concatenate([spot(s) for s in (sq, sk, sv, sg, so, sd, su)])[None, :]
        gains = jnp.stack([mix_gain, mlp_gain])
        cos_t, sin_t = tables(length, ret // heads, heads)
        own = [jnp.concatenate([w.astype(BF) for w in (wq, wk, wv, wg)], axis=1), wo.astype(BF).T]
        own.append(wu.astype(BF).reshape(-1, G, chunk).transpose(1, 0, 2))
        own.append(wd.astype(BF).reshape(G, chunk, -1).transpose(0, 2, 1))
        n_w = len(own)
        vm = pl.BlockSpec(memory_space=pltpu.VMEM)
        dma = pltpu.SemaphoreType.DMA
        tile = (length, width)
        scratch = [pltpu.VMEM((n_fs * w.shape[-2], w.shape[-1]), BF) for w in own]
        scratch += [
            pltpu.VMEM((n_fs,) + scales.shape, F32),
            pltpu.VMEM(scales.shape, F32),
            pltpu.VMEM((n_tp,) + tile, BF),
            pltpu.VMEM((G, n_tp) + tile, BF),
            pltpu.VMEM((G + 1, C, Y) + tile, BF),
            pltpu.VMEM((G + 1, C - 1, Y) + tile, BF),
            pltpu.VMEM((G + 1, Y) + tile, BF),
            pltpu.VMEM((G + 1, Y - 1) + tile, BF),
            pltpu.VMEM((G,) + tile, BF),
            pltpu.VMEM((G - 1,) + tile, BF),
            pltpu.VMEM((length, D), BF),
            pltpu.VMEM((4, length, ret), BF),
            pltpu.VMEM((length, ret), BF),
            pltpu.VMEM((G, length, chunk), BF),
            dma((n_w + 2,)),
        ]
        for shape in [(n_w + 1, Z - 1), (n_w + 1, Z, X - 1), (n_tp - 1,), (G - 1,), (G, Y - 1), (G, Y, C - 1),
                      (G + 1, C - 1), (G + 1, Y - 1), (G - 1,)]:
            scratch += [dma(shape), dma(shape)]
        out = pl.pallas_call(
            functools.partial(kernel, (Z, X, Y, C, G, heads)),
            out_shape=jax.ShapeDtypeStruct((length, width), BF),
            in_specs=[vm] * 5 + [pl.BlockSpec(memory_space=pltpu.SMEM)] + [vm] * n_w,
            out_specs=vm,
            scratch_shapes=scratch,
            compiler_params=pltpu.CompilerParams(
                collective_id=0, has_side_effects=True, vmem_limit_bytes=60 * 2**20
            ),
            name="layer",
        )(tokens.T, gains, scales, jnp.asarray(cos_t), jnp.asarray(sin_t), forget, *own)
        return out.T

    cut = P(("tp", "fs"))
    rows, cols = P("fs", "tp"), P("tp", "fs")
    in_specs = (cols, P(), P(), rows, rows, rows, rows, cols, rows, cols) + (cut,) * 7 + (P("tp"),)
    return jax.shard_map(on_device, mesh=mesh, in_specs=in_specs, out_specs=cols, check_vma=False)
```

```python
import functools

import jax
import jax.numpy as jnp
import numpy as np
from jax import lax
from jax.experimental import pallas as pl
from jax.experimental.pallas import tpu as pltpu
from jax.sharding import PartitionSpec as P

MESH = pl.DeviceIdType.MESH
BF = jnp.bfloat16
F32 = jnp.float32


def nn(a, b):
    return lax.dot_general(a, b, (((1,), (0,)), ((), ())), preferred_element_type=F32)


def nt(a, b):
    return lax.dot_general(a, b, (((1,), (1,)), ((), ())), preferred_element_type=F32)


def kernel(cfg, *refs):
    Z, X, Y, C, G, heads = cfg
    n_tp = Y * C
    n_w = 4
    tok, gains, scales, cos_t, sin_t, forget = refs[:6]
    own = refs[6 : 6 + n_w]
    out_ref = refs[6 + n_w]
    rest = refs[7 + n_w :]
    full = rest[:n_w]
    (scale_g, scale_row, tok_g, seqs, parts, core_in, y_out, y_in, z_out, z_in, normed, proj, mixed, hidden,
     local_sem, zs, zr, xs, xr, ts, tr, azs, azr, ays, ayr, acs, acr, rcs, rcr, rys, ryr, rzs, rzr) = rest[n_w:]
    me = lax.axis_index("fs")
    tp = lax.axis_index("tp")
    z = me // X
    x = lax.rem(me, X)
    y = tp // C
    core = lax.rem(tp, C)
    length, width = tok.shape
    ret = mixed.shape[1]
    head = ret // heads

    def at_z(o):
        return lax.rem(z + o, Z) * X + x

    def at_g(o):
        return (z // G * G + lax.rem(z + o, G)) * X + x

    def at_x(o):
        return z * X + lax.rem(x + o, X)

    def at_tp(o):
        return lax.rem(tp + o, n_tp)

    def at_y(o):
        return lax.rem(y + o, Y) * C + core

    def at_core(o):
        return y * C + lax.rem(core + o, C)

    barrier = pltpu.get_barrier_semaphore()
    for o in range(1, Z):
        pl.semaphore_signal(barrier, inc=1, device_id={"fs": at_z(o)}, device_id_type=MESH)
    for o in range(1, X):
        pl.semaphore_signal(barrier, inc=1, device_id={"fs": at_x(o)}, device_id_type=MESH)
    for o in range(1, n_tp):
        pl.semaphore_signal(barrier, inc=1, device_id={"tp": at_tp(o)}, device_id_type=MESH)
    pl.semaphore_wait(barrier, Z - 1 + X - 1 + n_tp - 1)

    pending = []

    def remote(src, dst, ss, rs, where):
        return pltpu.make_async_remote_copy(
            src_ref=src, dst_ref=dst, send_sem=ss, recv_sem=rs, device_id=where, device_id_type=MESH
        )

    def send(*parts_of):
        copy = remote(*parts_of)
        copy.start()
        pending.append(copy)

    def place(w, owner):
        if w == n_w:
            return scale_g.at[owner]
        rows = own[w].shape[-2]
        return full[w].at[pl.ds(pl.multiple_of(owner * rows, rows), rows)]

    def mine(w, o):
        if w == n_w:
            return scales
        return own[w].at[lax.rem(z + o, G)] if w >= 2 else own[w]

    def z_send(w):
        for o in range(1, Z):
            send(mine(w, o), place(w, me), zs.at[w, o - 1], zr.at[w, o - 1], {"fs": at_z(o)})

    def x_own(w):
        for o in range(1, X):
            send(mine(w, 0), place(w, me), xs.at[w, 0, o - 1], xr.at[w, 0, o - 1], {"fs": at_x(o)})

    def relay(w):
        for k in range(1, Z):
            piece = place(w, at_z(Z - k))
            remote(piece, piece, zs.at[w, k - 1], zr.at[w, k - 1], {"fs": at_z(k)}).wait_recv()
            for o in range(1, X):
                send(piece, piece, xs.at[w, k, o - 1], xr.at[w, k, o - 1], {"fs": at_x(o)})

    def finish(w):
        for k in range(Z):
            for o in range(1, X):
                owner = lax.rem(z + Z - k, Z) * X + lax.rem(x + X - o, X)
                piece = place(w, owner)
                remote(piece, piece, xs.at[w, k, o - 1], xr.at[w, k, o - 1], {"fs": at_x(o)}).wait_recv()

    def store_parts(k, t, value):
        parts[k, t % C, t // C] = value.astype(BF)

    def reduce_start(k):
        for o in range(1, C):
            send(parts.at[k, lax.rem(core + o, C)], core_in.at[k, o - 1], rcs.at[k, o - 1], rcr.at[k, o - 1],
                 {"tp": at_core(o)})

    def reduce_core(k):
        for o in range(1, C):
            slot = core_in.at[k, o - 1]
            remote(slot, slot, rcs.at[k, o - 1], rcr.at[k, o - 1], {"tp": at_core(o)}).wait_recv()
        for j in range(Y):
            value = parts[k, core, j].astype(F32)
            for o in range(1, C):
                value += core_in[k, o - 1, j].astype(F32)
            y_out[k, j] = value.astype(BF)
        for j in range(1, Y):
            send(y_out.at[k, lax.rem(y + j, Y)], y_in.at[k, j - 1], rys.at[k, j - 1], ryr.at[k, j - 1],
                 {"tp": at_y(j)})

    def reduce_y(k):
        value = y_out[k, y].astype(F32)
        for j in range(1, Y):
            slot = y_in.at[k, j - 1]
            remote(slot, slot, rys.at[k, j - 1], ryr.at[k, j - 1], {"tp": at_y(j)}).wait_recv()
            value += y_in[k, j - 1].astype(F32)
        return value

    def norm(block, row):
        square = jnp.zeros((length, 1), F32)
        for t in range(n_tp):
            v = block(t)[...].astype(F32)
            square += jnp.sum(v * v, axis=-1, keepdims=True)
        factor = lax.rsqrt(square / (width * n_tp) + 1e-6)
        for t in range(n_tp):
            cols = slice(t * width, (t + 1) * width)
            normed[:, cols] = (block(t)[...].astype(F32) * factor * gains[row : row + 1, cols]).astype(BF)

    for o in range(1, n_tp):
        send(tok, tok_g.at[tp], ts.at[o - 1], tr.at[o - 1], {"tp": at_tp(o)})
    for w in (n_w, 0, 1):
        z_send(w)
        x_own(w)
    locals_ = [pltpu.make_async_copy(mine(w, 0), place(w, me), local_sem.at[w]) for w in range(n_w + 1)]
    locals_.append(pltpu.make_async_copy(tok, tok_g.at[tp], local_sem.at[n_w + 1]))
    for copy in locals_:
        copy.start()
    for copy in locals_:
        copy.wait()
    for o in range(1, n_tp):
        slot = tok_g.at[at_tp(n_tp - o)]
        remote(slot, slot, ts.at[o - 1], tr.at[o - 1], {"tp": at_tp(o)}).wait_recv()
    norm(lambda t: tok_g.at[t], 0)

    relay(n_w)
    relay(0)
    relay(1)
    z_send(2)
    finish(n_w)
    finish(0)
    x_own(2)
    scale = jnp.sum(scale_g[...], axis=0)
    scale_row[...] = scale
    at = 4 * ret
    out_scale = scale[:, at : at + width]
    down_scale = scale[:, at + width : at + 2 * width]
    up_at = at + 2 * width

    for i in range(4):
        piece = nn(normed[...], full[0][:, i * ret : (i + 1) * ret])
        proj[i] = (piece * scale[:, i * ret : (i + 1) * ret]).astype(BF)

    r = lax.broadcasted_iota(jnp.int32, (ret, ret), 0)
    c = lax.broadcasted_iota(jnp.int32, (ret, ret), 1)
    odd = lax.rem(c, 2) == 1
    swap = jnp.where((r == c - 1) & odd, 1.0, jnp.where((r == c + 1) & ~odd, -1.0, 0.0)).astype(BF)
    same = jnp.where(r // head == c // head, 1.0 / head, 0.0).astype(F32)

    def turn(field):
        return field.astype(F32) * cos_t[...] + nn(field, swap) * sin_t[...]

    rot_q = turn(proj[0])
    rot_k = (turn(proj[1]) * head ** (-0.5)).astype(BF)
    vals = proj[2]
    rows = lax.broadcasted_iota(jnp.int32, (length, length), 0)
    cols = lax.broadcasted_iota(jnp.int32, (length, length), 1)
    dist = (rows - cols).astype(F32)
    lane = lax.broadcasted_iota(jnp.int32, (length, ret), 1) // head
    total = jnp.zeros((length, ret), F32)
    for h in range(heads):
        q_h = jnp.where(lane == h, rot_q, 0.0).astype(BF)
        decay = jnp.where(dist >= 0.0, jnp.exp(-forget[h] * jnp.maximum(dist, 0.0)), 0.0)
        inner = (nt(q_h, rot_k) * decay).astype(BF)
        total = jnp.where(lane == h, nn(inner, vals), total)
    mean = lax.dot_general(
        total * total, same, (((1,), (0,)), ((), ())), precision=lax.Precision.HIGHEST, preferred_element_type=F32
    )
    gate = proj[3].astype(F32)
    mixed[...] = (gate / (1.0 + jnp.exp(-gate)) * (total * lax.rsqrt(mean + 0.01))).astype(BF)

    finish(1)
    x_own(3)
    for t in range(n_tp):
        store_parts(G, t, nt(mixed[...], full[1][t * width : (t + 1) * width, :]))
    reduce_start(G)
    reduce_core(G)
    after = (tok[...].astype(F32) + reduce_y(G) * out_scale).astype(BF)
    seqs[0, tp] = after

    for k in range(1, G):
        send(seqs.at[0, tp], seqs.at[k, tp], azs.at[k - 1], azr.at[k - 1], {"fs": at_g(k)})

    def collect_z(k):
        slot = seqs.at[k, tp]
        if k:
            remote(slot, slot, azs.at[k - 1], azr.at[k - 1], {"fs": at_g(k)}).wait_recv()
        for j in range(1, Y):
            send(slot, slot, ays.at[k, j - 1], ayr.at[k, j - 1], {"tp": at_y(j)})
        for o in range(1, C):
            send(slot, slot, acs.at[k, 0, o - 1], acr.at[k, 0, o - 1], {"tp": at_core(o)})

    def collect_y(k):
        for j in range(1, Y):
            slot = seqs.at[k, at_y(Y - j)]
            remote(slot, slot, ays.at[k, j - 1], ayr.at[k, j - 1], {"tp": at_y(j)}).wait_recv()
            for o in range(1, C):
                send(slot, slot, acs.at[k, j, o - 1], acr.at[k, j, o - 1], {"tp": at_core(o)})

    def feed(k):
        for j in range(Y):
            for o in range(1, C):
                slot = seqs.at[k, lax.rem(y + Y - j, Y) * C + lax.rem(core + C - o, C)]
                remote(slot, slot, acs.at[k, j, o - 1], acr.at[k, j, o - 1], {"tp": at_core(o)}).wait_recv()
        norm(lambda t: seqs.at[k, t], 1)

    def expand(k):
        chunk = hidden.shape[2]
        step = 256 if chunk % 256 == 0 else chunk

        def tile(i, carry):
            here = pl.ds(pl.multiple_of(i * step, step), step)
            s = scale_row[:, pl.ds(pl.multiple_of(up_at + lax.rem(z, G) * chunk + i * step, 128), step)]
            u = jnp.maximum(nn(normed[...], full[2][:, here]) * s, 0.0)
            hidden[k, :, here] = (u * u).astype(BF)
            return carry

        lax.fori_loop(0, chunk // step, tile, 0)

    def shrink(k):
        for t in range(n_tp):
            store_parts(k, t, nt(hidden[k], full[3][t * width : (t + 1) * width, :]))
        reduce_start(k)

    def give_z(k):
        value = reduce_y(k)
        z_out[k] = value.astype(BF)
        if k:
            send(z_out.at[k], z_in.at[k - 1], rzs.at[k - 1], rzr.at[k - 1], {"fs": at_g(G - k)})

    collect_z(0)
    relay(2)
    for k in range(1, G):
        collect_z(k)
    z_send(3)
    collect_y(0)
    feed(0)
    finish(2)
    expand(0)
    for k in range(1, G):
        collect_y(k)
        feed(k)
        expand(k)
    relay(3)
    finish(3)
    order = list(range(1, G)) + [0]
    for k in order:
        shrink(k)
    for k in order:
        reduce_core(k)
    for k in order:
        give_z(k)
    mlp_total = z_out[0].astype(F32)
    for k in range(1, G):
        slot = z_in.at[k - 1]
        remote(slot, slot, rzs.at[k - 1], rzr.at[k - 1], {"fs": at_g(k)}).wait_recv()
        mlp_total += z_in[k - 1].astype(F32)
    out_ref[...] = (seqs[0, tp].astype(F32) + mlp_total * down_scale).astype(BF)
    for copy in pending:
        copy.wait_send()


def tables(length, head, heads):
    half = head // 2
    inverse = 1.0 / 10000.0 ** np.linspace(0.0, 1.0, half)
    angle = np.arange(length)[:, None] * inverse.astype(np.float32).astype(np.float64)[None, :]
    spread = lambda a: np.tile(np.repeat(a, 2, axis=1), (1, heads)).astype(np.float32)
    return spread(np.cos(angle)), spread(np.sin(angle))


def solution(mesh):
    n_fs, n_tp = mesh.shape["fs"], mesh.shape["tp"]
    heights = [getattr(d, "coords", (0, 0, i))[2] for i, d in enumerate(mesh.devices[:, 0])]
    X = heights.count(heights[0])
    if n_fs % X:
        X = 1
    Z = n_fs // X
    cores = [getattr(d, "core_on_chip", 0) for d in mesh.devices[0]]
    C = len(set(cores))
    if n_tp % C:
        C = 1
    Y = n_tp // C
    G = 2 if Z % 2 == 0 else Z

    def on_device(tokens, mix_gain, mlp_gain, wq, wk, wv, wg, wo, wu, wd, sq, sk, sv, sg, so, su, sd, forget):
        width, length = tokens.shape
        D = width * n_tp
        ret = wq.shape[1]
        heads = forget.shape[0]
        ff = wu.shape[1]
        chunk = ff // G
        me = lax.axis_index("fs")

        def spot(s):
            wide = jnp.tile(s, n_fs)
            return jnp.where(jnp.arange(wide.shape[0]) // s.shape[0] == me, wide, 0.0)

        scales = jnp.concatenate([spot(s) for s in (sq, sk, sv, sg, so, sd, su)])[None, :]
        gains = jnp.stack([mix_gain, mlp_gain])
        cos_t, sin_t = tables(length, ret // heads, heads)
        own = [jnp.concatenate([w.astype(BF) for w in (wq, wk, wv, wg)], axis=1), wo.astype(BF).T]
        own.append(wu.astype(BF).reshape(-1, G, chunk).transpose(1, 0, 2))
        own.append(wd.astype(BF).reshape(G, chunk, -1).transpose(0, 2, 1))
        n_w = len(own)
        vm = pl.BlockSpec(memory_space=pltpu.VMEM)
        dma = pltpu.SemaphoreType.DMA
        tile = (length, width)
        scratch = [pltpu.VMEM((n_fs * w.shape[-2], w.shape[-1]), BF) for w in own]
        scratch += [
            pltpu.VMEM((n_fs,) + scales.shape, F32),
            pltpu.VMEM(scales.shape, F32),
            pltpu.VMEM((n_tp,) + tile, BF),
            pltpu.VMEM((G, n_tp) + tile, BF),
            pltpu.VMEM((G + 1, C, Y) + tile, BF),
            pltpu.VMEM((G + 1, C - 1, Y) + tile, BF),
            pltpu.VMEM((G + 1, Y) + tile, BF),
            pltpu.VMEM((G + 1, Y - 1) + tile, BF),
            pltpu.VMEM((G,) + tile, BF),
            pltpu.VMEM((G - 1,) + tile, BF),
            pltpu.VMEM((length, D), BF),
            pltpu.VMEM((4, length, ret), BF),
            pltpu.VMEM((length, ret), BF),
            pltpu.VMEM((G, length, chunk), BF),
            dma((n_w + 2,)),
        ]
        for shape in [(n_w + 1, Z - 1), (n_w + 1, Z, X - 1), (n_tp - 1,), (G - 1,), (G, Y - 1), (G, Y, C - 1),
                      (G + 1, C - 1), (G + 1, Y - 1), (G - 1,)]:
            scratch += [dma(shape), dma(shape)]
        out = pl.pallas_call(
            functools.partial(kernel, (Z, X, Y, C, G, heads)),
            out_shape=jax.ShapeDtypeStruct((length, width), BF),
            in_specs=[vm] * 5 + [pl.BlockSpec(memory_space=pltpu.SMEM)] + [vm] * n_w,
            out_specs=vm,
            scratch_shapes=scratch,
            compiler_params=pltpu.CompilerParams(
                collective_id=0, has_side_effects=True, vmem_limit_bytes=60 * 2**20
            ),
            name="layer",
        )(tokens.T, gains, scales, jnp.asarray(cos_t), jnp.asarray(sin_t), forget, *own)
        return out.T

    cut = P(("tp", "fs"))
    rows, cols = P("fs", "tp"), P("tp", "fs")
    in_specs = (cols, P(), P(), rows, rows, rows, rows, cols, rows, cols) + (cut,) * 7 + (P("tp"),)
    return jax.shard_map(on_device, mesh=mesh, in_specs=in_specs, out_specs=cols, check_vma=False)
```
